512 devices in a mesh: ep: 32 (over z, x), tp: 16 (over y, core).
Axes of the slice: x: 4, y: 8, z: 8, core: 2. Of those that a mesh axis runs over, the one named last changes fastest.
Arguments:
- tokens: bfloat16 [16384, 4096], P('ep', 'tp'), may hold values from -6 to 6
- cotangent: bfloat16 [16384, 4096], P('ep', 'tp'), may hold values from -6 to 6
- expert_ids: int32 [16384, 2], P('ep'), may hold values from 0 to 63, as said below
- route_weight: float32 [16384, 2], P('ep'), may hold values from 0.1 to 1
- gate_weight: bfloat16 [64, 4096, 512], P('ep', 'tp'), may hold values from -0.09375 to 0.09375
- up_weight: bfloat16 [64, 4096, 512], P('ep', 'tp'), may hold values from -0.09375 to 0.09375
- down_weight: bfloat16 [64, 512, 4096], P('ep', None, 'tp'), may hold values from -0.25 to 0.25
- saved_gate: bfloat16 [32, 64, 32, 512], P(None, 'ep'), may hold values from -6 to 6
- saved_up: bfloat16 [32, 64, 32, 512], P(None, 'ep'), may hold values from -6 to 6
Outputs:
- token_grad: bfloat16 [16384, 4096], P('ep', 'tp')
- route_grad: float32 [16384, 2], P('ep')
- gate_weight_grad: bfloat16 [64, 4096, 512], P('ep', 'tp')
- up_weight_grad: bfloat16 [64, 4096, 512], P('ep', 'tp')
- down_weight_grad: bfloat16 [64, 512, 4096], P('ep', None, 'tp')
The draws below stay inside these ranges and needn't reach their ends.
Inputs may be any that keep to these rules, and one draw needn't show every extreme that they name: `expert_ids`: each row names 2 different experts of one group of 4 consecutive experts. In each aligned block of 512 rows (the rows of one index of ep) no expert is named more than 32 times; the experts of one group, drawn from the seed, are named exactly 32 times in every block, and other experts may reach 32 too.
All inputs are finite; a program needn't handle non-finite values.
Results may differ from the reference program's by a relative error of at most 0.02.
Values may be sent and summed in bfloat16 or wider, within the bound.
A program may use at most 64 MiB of HBM per device.

```python
import jax
import jax.numpy as jnp
from jax import lax

D = 4096
F = 512
TOP_K = 2
E_GROUP = 4
TOK_DEV = 512
BLOCKS = 32
EXPERTS = 64
GROUPS = 16
CAP = 32
TOKENS = 16384
N_TP = 16


def block_choices(block_key, hot_group):
    first_key, second_key, third_key, fourth_key, fifth_key = jax.random.split(block_key, 5)
    offsets = jax.random.randint(first_key, (GROUPS,), 0, E_GROUP)
    second_group = (hot_group + 1 + jax.random.randint(second_key, (), 0, GROUPS - 1)) % GROUPS
    group_range = jnp.arange(GROUPS, dtype=jnp.int32)
    taken = ((group_range == hot_group) | (group_range == second_group)).astype(jnp.int32)
    order_keys = jax.random.permutation(third_key, GROUPS).astype(jnp.int32) + GROUPS * taken
    ranked = jnp.argsort(order_keys).astype(jnp.int32)
    rest_groups = ranked[:GROUPS - 2]
    busiest = CAP * E_GROUP // 2
    places = jnp.arange(TOK_DEV, dtype=jnp.int32)
    remain = jnp.maximum(places - 2 * busiest, 0)
    spread_group = rest_groups[remain % (GROUPS - 2)]
    group = jnp.where(places < busiest, hot_group, jnp.where(places < 2 * busiest, second_group, spread_group))
    inner = jnp.where(places < 2 * busiest, places % busiest, remain // (GROUPS - 2))
    first = group * E_GROUP + (inner + offsets[group]) % E_GROUP
    second = group * E_GROUP + (inner + 1 + offsets[group]) % E_GROUP
    flips = jax.random.randint(fourth_key, (TOK_DEV,), 0, 2)
    paired = jnp.stack([jnp.where(flips == 1, second, first), jnp.where(flips == 1, first, second)], axis=1)
    shuffle = jax.random.permutation(fifth_key, TOK_DEV)
    return paired[shuffle]


def draw_expert_ids(key, part):
    hot_group = jax.random.randint(jax.random.fold_in(key, 11), (), 0, GROUPS)
    block_keys = jax.random.split(jax.random.fold_in(key, 12), TOKENS // TOK_DEV)
    chosen = jax.vmap(lambda block_key: block_choices(block_key, hot_group))(block_keys)
    return chosen.reshape(TOKENS, TOP_K).astype(jnp.int32)


def shard_levels(stream_key, dims, pieces, least, top_value):
    loudness = 1.0
    for dim, parts in pieces:
        heights = jax.random.uniform(jax.random.fold_in(jax.random.fold_in(stream_key, 6), dim), (parts,), jnp.float32, least / len(pieces), top_value / len(pieces))
        loudness = loudness * jnp.repeat(jnp.exp(heights), dims[dim] // parts).reshape((-1,) + (1,) * (len(dims) - 1 - dim))
    return loudness


def scatter_about(key, dims, spread, reach, shards=(), held_as=jnp.bfloat16):
    gain = shard_levels(key, dims, shards, -0.22, 0.18) if shards else 1.0
    values = jax.random.normal(key, dims, jnp.float32) * spread * gain
    return jnp.minimum(jnp.maximum(values, -reach), reach).astype(held_as)


def setup_inputs(seed: int = 0) -> dict:
    seeds = jax.random.split(jax.random.key(seed), 10)
    return {
        "tokens": scatter_about(seeds[0], (TOKENS, D), 1.0, 6.0, ((0, 32), (1, 16))),
        "cotangent": scatter_about(seeds[1], (TOKENS, D), 1.0, 6.0, ((0, 32), (1, 16))),
        "expert_ids": draw_expert_ids(jax.random.fold_in(seeds[9], 71), 0),
        "route_weight": jnp.clip(0.1 + 0.9 * jax.random.uniform(seeds[3], (TOKENS, TOP_K), jnp.float32) ** shard_levels(seeds[3], (TOKENS, TOP_K), ((0, 32),), -0.2, 0.2), 0.1, 1.0),
        "gate_weight": scatter_about(seeds[4], (EXPERTS, D, F), D ** -0.5, 0.09375, ((0, 32), (1, 16))),
        "up_weight": scatter_about(seeds[5], (EXPERTS, D, F), D ** -0.5, 0.09375, ((0, 32), (1, 16))),
        "down_weight": scatter_about(seeds[6], (EXPERTS, F, D), F ** -0.5, 0.25, ((0, 32), (2, 16))),
        "saved_gate": scatter_about(seeds[7], (BLOCKS, EXPERTS, CAP, F), 1.5, 6.0, ((1, 32),)),
        "saved_up": scatter_about(seeds[8], (BLOCKS, EXPERTS, CAP, F), 1.0, 6.0, ((1, 32),)),
    }


def slot_layout(expert_ids):
    assigned = TOK_DEV * TOP_K
    flat_ids = expert_ids.reshape(BLOCKS, assigned)
    onehot = (flat_ids[:, :, None] == jnp.arange(EXPERTS, dtype=jnp.int32)[None, None, :]).astype(jnp.int32)
    earlier = jnp.cumsum(onehot, axis=1) - onehot
    slot_index = jnp.sum(earlier * onehot, axis=2).astype(jnp.int32)
    position = (flat_ids * CAP + slot_index).astype(jnp.int32)
    block_index = jnp.broadcast_to(jnp.arange(BLOCKS, dtype=jnp.int32)[:, None], (BLOCKS, assigned))
    numbers = jnp.broadcast_to(jnp.arange(assigned, dtype=jnp.int32)[None, :], (BLOCKS, assigned))
    slot_table = jnp.full((BLOCKS, EXPERTS * CAP), assigned, jnp.int32).at[block_index, position].set(numbers)
    return position, slot_table


def reference(tokens, cotangent, expert_ids, route_weight, gate_weight, up_weight, down_weight, saved_gate, saved_up):
    assigned = TOK_DEV * TOP_K
    model_width = tokens.shape[1]
    hidden_units = gate_weight.shape[2]
    width_local = model_width // N_TP
    position, slot_table = slot_layout(expert_ids)
    filled = slot_table < assigned
    picked = jnp.minimum(slot_table, assigned - 1)
    block_base = jnp.arange(BLOCKS, dtype=jnp.int32)[:, None]
    token_row = jnp.where(filled, block_base * TOK_DEV + picked // TOP_K, TOKENS).astype(jnp.int32)
    slot_weight = jnp.where(filled, route_weight.reshape(-1)[block_base * assigned + picked], jnp.float32(0.0))
    token_row = jnp.transpose(token_row.reshape(BLOCKS, EXPERTS, CAP), (1, 0, 2))
    slot_weight = jnp.transpose(slot_weight.reshape(BLOCKS, EXPERTS, CAP), (1, 0, 2))
    padded_tokens = jnp.concatenate([tokens, jnp.zeros((1, model_width), tokens.dtype)], axis=0)
    padded_cot = jnp.concatenate([cotangent, jnp.zeros((1, model_width), cotangent.dtype)], axis=0)
    gate_saved = jnp.transpose(saved_gate, (1, 0, 2, 3))
    up_saved = jnp.transpose(saved_up, (1, 0, 2, 3))

    def expert_step(totals, inputs):
        gate_one, up_one, down_one, pre_gate, pre_up, row_index, weight_slot = inputs
        rows_flat = row_index.reshape(-1)
        inputs_rows = padded_tokens[rows_flat]
        grads_in = padded_cot[rows_flat]
        gate_pre = pre_gate.astype(jnp.float32).reshape(-1, hidden_units)
        up_pre = pre_up.astype(jnp.float32).reshape(-1, hidden_units)
        sigmoid_gate = jax.nn.sigmoid(gate_pre)
        hidden = gate_pre * sigmoid_gate * up_pre
        hidden_bf = hidden.astype(jnp.bfloat16)
        partial_terms = jnp.einsum("rnd,fnd->rnf",
                                   grads_in.reshape(-1, N_TP, width_local).astype(jnp.float32),
                                   down_one.reshape(hidden_units, N_TP, width_local).astype(jnp.float32))
        rounded = lax.optimization_barrier(partial_terms.astype(jnp.bfloat16))
        back_grad = jnp.sum(rounded.astype(jnp.float32), axis=1)
        expert_out = jnp.dot(hidden_bf, down_one, preferred_element_type=jnp.float32)
        scores = jnp.sum(expert_out * grads_in.astype(jnp.float32), axis=1)
        weights = weight_slot.reshape(-1)[:, None]
        grad_hidden = weights * back_grad
        grad_up_pre = (grad_hidden * gate_pre * sigmoid_gate).astype(jnp.bfloat16)
        grad_gate_pre = (grad_hidden * up_pre * sigmoid_gate * (1.0 + gate_pre * (1.0 - sigmoid_gate))).astype(jnp.bfloat16)
        weighted = (weights * hidden).astype(jnp.bfloat16)
        gate_grad_one = jnp.dot(inputs_rows.T, grad_gate_pre, preferred_element_type=jnp.float32).astype(jnp.bfloat16)
        up_grad_one = jnp.dot(inputs_rows.T, grad_up_pre, preferred_element_type=jnp.float32).astype(jnp.bfloat16)
        down_grad_one = jnp.dot(weighted.T, grads_in, preferred_element_type=jnp.float32).astype(jnp.bfloat16)
        slot_grad = (jnp.dot(grad_gate_pre, gate_one.T, preferred_element_type=jnp.float32)
                     + jnp.dot(grad_up_pre, up_one.T, preferred_element_type=jnp.float32)).astype(jnp.bfloat16)
        totals = totals.at[rows_flat].add(slot_grad.astype(jnp.float32))
        return totals, (gate_grad_one, up_grad_one, down_grad_one, scores)

    initial = jnp.zeros((TOKENS + 1, model_width), jnp.float32)
    totals, outputs = lax.scan(expert_step, initial,
                               (gate_weight, up_weight, down_weight, gate_saved, up_saved, token_row, slot_weight))
    gate_weight_grad, up_weight_grad, down_weight_grad, scores = outputs
    token_grad = totals[:TOKENS].astype(jnp.bfloat16)
    score_table = jnp.transpose(scores.reshape(EXPERTS, BLOCKS, CAP), (1, 0, 2)).reshape(BLOCKS, EXPERTS * CAP)
    route_grad = jnp.take_along_axis(score_table, position, axis=1).reshape(TOKENS, TOP_K)
    return token_grad, route_grad, gate_weight_grad, up_weight_grad, down_weight_grad
```

```python
import functools

import jax
import jax.numpy as jnp
from jax import lax
from jax.experimental import pallas as pl
from jax.experimental.pallas import tpu as pltpu
from jax.sharding import Mesh
from jax.sharding import PartitionSpec as P

EP = ("z", "x")
TP = ("y", "c")
NX = 4
CAP = 32
SEATS = 64
ROWS = NX * CAP
F32 = jnp.float32
BF16 = jnp.bfloat16
DY, XT, META = 0, 1, 2


def dot(a, b, ca=1, cb=0):
    return lax.dot_general(a, b, (((ca,), (cb,)), ((), ())), preferred_element_type=F32)


def kernel(
    nz, ids_ref, rw_ref, tok_ref, cot_ref, gate_hbm, up_hbm, down_hbm, sg_hbm, su_hbm,
    tg_ref, rg_ref, gg_ref, ug_ref, dg_ref,
    gate, up, down, sg, su, pre_u, pre_g, hid, pw, gmat,
    sz, szm, rz, rzm, rx, rxm, perm, wcol, slots,
    zp, zr, rss, rsr, zf, du, dg, ts, tsm, cx, cxm, bs, bsm, br, brm,
    lsem, zss, zrs, xss, xrs, pss, prs, rcs, rcr, acs, acr, qss, qrs, vss, vrs, wss, wrs,
):
    zi, xi, yi, ci = (lax.axis_index(a) for a in ("z", "x", "y", "c"))
    ny = nz
    hf = zf.shape[-1]
    tokens = tok_ref.shape[0]
    left_half = lax.div(xi, 2) == 0
    my_row = 2 * lax.rem(xi, 2)
    seat0 = pl.multiple_of(SEATS * lax.div(xi, 2), SEATS)

    def far_first(k):
        k2 = nz - k
        return jnp.where(lax.rem(k2, 2) == 1, lax.div(k2 + 1, 2), nz - lax.div(k2, 2))

    def remote(src, dst, ssem, rsem, **where):
        return pltpu.make_async_remote_copy(
            src_ref=src, dst_ref=dst, send_sem=ssem, recv_sem=rsem,
            device_id=where, device_id_type=pl.DeviceIdType.MESH,
        )

    loads = [
        pltpu.make_async_copy(src, dst, lsem.at[i])
        for i, (src, dst) in enumerate(
            ((sg_hbm, sg), (su_hbm, su), (down_hbm, down), (gate_hbm, gate), (up_hbm, up))
        )
    ]
    for copy in loads:
        copy.start()

    barrier = pltpu.get_barrier_semaphore()

    def greet(**where):
        pl.semaphore_signal(barrier, 1, device_id=where, device_id_type=pl.DeviceIdType.MESH)

    for k in range(1, nz):
        greet(z=lax.rem(zi + k, nz))
    for k in range(1, NX):
        greet(x=lax.rem(xi + k, NX))
    greet(y=lax.rem(yi + 1, ny))
    greet(y=lax.rem(yi + ny - 1, ny))
    greet(c=1 - ci)

    experts, groups = 4 * 2 * nz, 2 * nz
    id0, id1 = ids_ref[0:1, :], ids_ref[1:2, :]
    rw0, rw1 = rw_ref[0:1, :], rw_ref[1:2, :]
    group = lax.shift_right_logical(id0, 2)
    erow = lax.broadcasted_iota(jnp.int32, (experts, tokens), 0)
    hot0, hot1 = erow == id0, erow == id1
    chosen = jnp.where(hot0, 1.0, 0.0) + jnp.where(hot1, 1.0, 0.0)
    grow = lax.broadcasted_iota(jnp.int32, (groups, tokens), 0)
    ingroup = jnp.where(grow == group, 1.0, 0.0)
    earlier = jnp.where(
        lax.broadcasted_iota(jnp.int32, (tokens, tokens), 0)
        < lax.broadcasted_iota(jnp.int32, (tokens, tokens), 1),
        1.0, 0.0,
    ).astype(BF16)
    count = dot(jnp.concatenate([chosen, ingroup], axis=0).astype(BF16), earlier)
    rank = jnp.sum(ingroup * count[experts:], axis=0, keepdims=True)
    target = group * SEATS + rank.astype(jnp.int32)
    weight = jnp.where(hot0, rw0, 0.0) + jnp.where(hot1, rw1, 0.0)
    weight_hi = weight.astype(BF16).astype(F32)
    pw[0] = chosen * (count[:experts] + 1.0)
    pw[1] = weight_hi
    pw[2] = weight - weight_hi

    def seat_rows(zt):
        row = lax.broadcasted_iota(jnp.int32, (2 * SEATS, tokens), 0) + zt * (2 * SEATS)
        return jnp.where(row == target, 1.0, 0.0).astype(BF16)

    def gathered(zt):
        g = seat_rows(zt)
        gmat[pl.ds(pl.multiple_of(zt * 2 * SEATS, 2 * SEATS), 2 * SEATS), :] = g
        e0 = pl.multiple_of(zt * 8, 8)
        lhs = jnp.concatenate([pw[i, pl.ds(e0, 8), :] for i in range(3)], axis=0).astype(BF16)
        r = dot(lhs, g, 1, 1)
        tile = jnp.concatenate(
            [r[0:4] + r[4:8], (r[8:12] + r[12:16]) + (r[16:20] + r[20:24])], axis=0
        )
        return dot(g, cot_ref[...]).astype(BF16), tile

    rows, tile = gathered(zi)
    rz[DY, zi] = rows
    rzm[zi] = tile
    pl.semaphore_wait(barrier, (nz - 1) + (NX - 1) + 3)

    def z_copy(which, zt, zs):
        if which == META:
            return remote(szm.at[zt], rzm.at[zs], zss.at[META, zt], zrs.at[META, zs], z=zt)
        return remote(sz.at[which, zt], rz.at[which, zs], zss.at[which, zt], zrs.at[which, zs], z=zt)

    def send_dy(k, _):
        zt = lax.rem(zi + far_first(k), nz)
        rows, tile = gathered(zt)
        szm[zt] = tile
        sz[DY, zt] = rows
        z_copy(META, zt, zi).start()
        z_copy(DY, zt, zi).start()
        return 0

    lax.fori_loop(1, nz, send_dy, 0)

    def rows_of_tokens(zt):
        g = gmat[pl.ds(pl.multiple_of(zt * 2 * SEATS, 2 * SEATS), 2 * SEATS), :]
        return dot(g, tok_ref[...]).astype(BF16)

    def send_x(k, _):
        zt = lax.rem(zi + far_first(k), nz)
        sz[XT, zt] = rows_of_tokens(zt)
        z_copy(XT, zt, zi).start()
        return 0

    lax.fori_loop(1, nz, send_x, 0)
    rz[XT, zi] = rows_of_tokens(zi)

    loads[0].wait()
    loads[1].wait()

    def elementwise(i, _):
        q, j = lax.div(i, 2), lax.rem(i, 2)
        g = sg[pl.ds(NX * q, NX), j].astype(F32).reshape(ROWS, -1)
        u = su[pl.ds(NX * q, NX), j].astype(F32).reshape(ROWS, -1)
        s = jax.nn.sigmoid(g)
        gs = g * s
        pre_u[j, q] = gs
        pre_g[j, q] = u * s * (1.0 + g * (1.0 - s))
        hid[j, q] = gs * u
        return 0

    lax.fori_loop(0, 2 * nz, elementwise, 0)

    def came(k):
        return jnp.where(k == 0, zi, lax.rem(zi + nz - far_first(jnp.maximum(k, 1)), nz))

    def x_copy(which, q, xt, xs):
        if which == META:
            return remote(rzm.at[q], rxm.at[q, xs], xss.at[META, q, xt], xrs.at[META, q, xs], x=xt)
        seats = pl.ds(pl.multiple_of(SEATS * lax.div(xt, 2), SEATS), SEATS)
        return remote(
            rz.at[which, q, seats], rx.at[which, q, xs],
            xss.at[which, q, xt], xrs.at[which, q, xs], x=xt,
        )

    def spread(which, q):
        for d in range(1, NX):
            x_copy(which, q, lax.rem(xi + d, NX), xi).start()

    def pass_dy(q):
        spread(META, q)
        spread(DY, q)
        rx[DY, q, xi] = rz[DY, q, pl.ds(seat0, SEATS), :]
        rxm[q, xi] = rzm[q]

    def take_dy(k):
        q = came(k)
        z_copy(META, q, q).wait_recv()
        z_copy(DY, q, q).wait_recv()
        pass_dy(q)

    loads[2].wait()

    def pair_copy(q):
        return remote(zp.at[q, 1 - ci], zr.at[q], pss.at[q], prs.at[q], c=1 - ci)

    def back_partial(k):
        q = came(k)
        for d in range(1, NX):
            xs = lax.rem(xi + d, NX)
            x_copy(META, q, xs, xs).wait_recv()
            x_copy(DY, q, xs, xs).wait_recv()
        t = rxm[q]
        t = jnp.where(left_half, t[:, :, :SEATS], t[:, :, SEATS:])
        line = lax.broadcasted_iota(jnp.int32, t.shape, 1)

        def lanes(i):
            v = jnp.sum(jnp.where(line == i, t, 0.0), axis=1)
            return jnp.concatenate([v[n : n + 1] for n in range(NX)], axis=1)

        base = CAP * lax.div(lax.broadcasted_iota(jnp.int32, (1, NX * SEATS), 1), SEATS)
        slot = lax.broadcasted_iota(jnp.int32, (ROWS, NX * SEATS), 0)
        for j in range(2):
            place = lanes(my_row + j).astype(jnp.int32)
            key = jnp.where(place > 0, place - 1 + base, -1)
            hit = slot == key
            perm[q, pl.ds(j * ROWS, ROWS), :] = jnp.where(hit, 1.0, 0.0).astype(BF16)
            w = jnp.sum(jnp.where(hit, lanes(4 + my_row + j), 0.0), axis=1, keepdims=True)
            wcol[j, q] = jnp.broadcast_to(w, (ROWS, 128))
        arrived = rx[DY, q].reshape(NX * SEATS, -1)
        moved = dot(perm[q], arrived).astype(BF16)
        for j in range(2):
            part = moved[j * ROWS : (j + 1) * ROWS]
            slots[DY, j, q] = part
            z = dot(part, down[j], 1, 1).astype(BF16)
            zp[q, 0, j] = z[:, :hf]
            zp[q, 1, j] = z[:, hf:]
        pair_copy(q).start()

    pass_dy(zi)
    lag = 2 if nz > 2 else 1
    for k in range(1, lag):
        take_dy(jnp.int32(k))

    def steady(k, _):
        take_dy(k)
        back_partial(k - lag)
        return 0

    lax.fori_loop(lag, nz, steady, 0)

    def rest(k, _):
        back_partial(k)
        return 0

    lax.fori_loop(nz - lag, nz, rest, 0)

    def wait_pair(q, _):
        pair_copy(q).wait_recv()
        return 0

    lax.fori_loop(0, nz, wait_pair, 0)

    hops = {(0, 0): ny // 2, (0, 1): ny - 1 - ny // 2, (1, 0): ny - 1 - ny // 2, (1, 1): ny // 2}
    flows = [f for f in hops]

    def at_y(d):
        return lax.rem(yi + d + 2 * ny, ny)

    def own(q, j):
        return zp[q, ci, j].astype(F32) + zr[q, j].astype(F32)

    def rs_copy(j, way, s):
        step = 1 - 2 * way
        return remote(
            rss.at[j, way, s - 1], rsr.at[j, way, s - 1],
            rcs.at[j, way, s - 1], rcr.at[j, way, s - 1], y=at_y(step),
        )

    for s in range(1, ny // 2 + 1):
        for j, way in flows:
            if s > hops[j, way]:
                continue
            total = own(at_y((1 - 2 * way) * (hops[j, way] + 1 - s)), j)
            if s > 1:
                rs_copy(j, way, s - 1).wait_recv()
                total = total + rsr[j, way, s - 2].astype(F32)
            rss[j, way, s - 1] = total.astype(BF16)
            rs_copy(j, way, s).start()
        if s == 1:
            def down_grads(j, _):
                def weigh(q, _):
                    w = jnp.concatenate([wcol[j, q]] * (hid.shape[-1] // 128), axis=1)
                    du[j, q] = (w * hid[j, q]).astype(BF16)
                    return 0

                lax.fori_loop(0, nz, weigh, 0)
                hw = du[j].reshape(nz * ROWS, -1)
                dy = slots[DY, j].reshape(nz * ROWS, -1)
                dg_ref[j] = dot(hw, dy, 0, 0).astype(BF16)
                return 0

            lax.fori_loop(0, 2, down_grads, 0)

    for j in range(2):
        total = own(yi, j)
        for way in range(2):
            if hops[j, way] > 0:
                rs_copy(j, way, hops[j, way]).wait_recv()
                total = total + rsr[j, way, hops[j, way] - 1].astype(F32)
        zf[yi, ci, j] = total.astype(BF16)

    def ag_copy(j, way, s):
        step = 1 - 2 * way
        q = at_y(-step * (s - 1))
        return remote(
            zf.at[q, ci, j], zf.at[q, ci, j],
            acs.at[j, way, s - 1], acr.at[j, way, s - 1], y=at_y(step),
        )

    def ag_wait(j, way, s):
        q = at_y(-(1 - 2 * way) * s)
        remote(
            zf.at[q, ci, j], zf.at[q, ci, j],
            acs.at[j, way, s - 1], acr.at[j, way, s - 1], y=yi,
        ).wait_recv()
        return q

    def half_copy(q, j, h):
        return remote(zf.at[q, h, j], zf.at[q, h, j], qss.at[q, j], qrs.at[q, j], c=1 - ci)

    for j, way in flows:
        if hops[j, way] > 0:
            ag_copy(j, way, 1).start()
    for j in range(2):
        half_copy(yi, j, ci).start()

    def take_x(q, _):
        @pl.when(q != zi)
        def _():
            z_copy(XT, q, q).wait_recv()

        spread(XT, q)
        rx[XT, q, xi] = rz[XT, q, pl.ds(seat0, SEATS), :]
        return 0

    lax.fori_loop(0, nz, take_x, 0)
    loads[3].wait()
    loads[4].wait()

    def back_copy(q, xt, xs):
        return remote(ts.at[q, xt], cx.at[q, xs], vss.at[0, q, xt], vrs.at[0, q, xs], x=xt)

    def back_meta(q, xt, xs):
        return remote(tsm.at[q, xt], cxm.at[q, xs], vss.at[1, q, xt], vrs.at[1, q, xs], x=xt)

    def consume(q):
        for j in range(2):
            half_copy(q, j, 1 - ci).wait_recv()
        grads, tiles = [], None
        line = lax.broadcasted_iota(jnp.int32, (8, 2 * SEATS), 0)
        side = lax.div(lax.broadcasted_iota(jnp.int32, (8, 2 * SEATS), 1), SEATS) == lax.div(xi, 2)
        for j in range(2):
            z = jnp.concatenate([zf[q, 0, j], zf[q, 1, j]], axis=1).astype(F32)
            w = jnp.concatenate([wcol[j, q]] * (z.shape[-1] // 128), axis=1)
            wz = w * z
            up_grad = (wz * pre_u[j, q]).astype(BF16)
            gate_grad = (wz * pre_g[j, q]).astype(BF16)
            du[j, q] = up_grad
            dg[j, q] = gate_grad
            hb = hid[j, q].astype(BF16).astype(F32)
            score = jnp.sum(hb * z, axis=1, keepdims=True)
            p = perm[q, pl.ds(j * ROWS, ROWS), :].astype(F32)
            seat_score = jnp.sum(p * score, axis=0, keepdims=True)
            s = dot(gate_grad, gate[j], 1, 1) + dot(up_grad, up[j], 1, 1)
            grads.append(s.astype(BF16))
            mask = side & (line == my_row + j)
            made = []
            for n in range(NX):
                one = seat_score[:, n * SEATS : (n + 1) * SEATS]
                made.append(jnp.where(mask, jnp.concatenate([one, one], axis=1), 0.0))
            tiles = made if tiles is None else [a + b for a, b in zip(tiles, made)]
        for n in range(NX):
            tsm[q, n] = tiles[n]
        t = dot(perm[q], jnp.concatenate(grads, axis=0), 0, 0).astype(BF16)
        ts[q] = t.reshape(NX, SEATS, -1)
        for d in range(1, NX):
            xt = lax.rem(xi + d, NX)
            back_meta(q, xt, xi).start()
            back_copy(q, xt, xi).start()
        cx[q, xi] = ts[q, xi]
        cxm[q, xi] = tsm[q, xi]

    def home_copy(q, zs):
        return remote(bs.at[q], br.at[zs], wss.at[0, q], wrs.at[0, zs], z=q)

    def home_meta(q, zs):
        return remote(bsm.at[q], brm.at[zs], wss.at[1, q], wrs.at[1, zs], z=q)

    def combine(q):
        for d in range(1, NX):
            xs = lax.rem(xi + d, NX)
            back_meta(q, xs, xs).wait_recv()
            back_copy(q, xs, xs).wait_recv()
        first = (cx[q, 0].astype(F32) + cx[q, 1].astype(F32)).astype(BF16)
        second = (cx[q, 2].astype(F32) + cx[q, 3].astype(F32)).astype(BF16)
        scores = (cxm[q, 0] + cxm[q, 1]) + (cxm[q, 2] + cxm[q, 3])

        @pl.when(q == zi)
        def _():
            br[q, pl.ds(0, SEATS), :] = first
            br[q, pl.ds(SEATS, SEATS), :] = second
            brm[q] = scores

        @pl.when(q != zi)
        def _():
            bs[q, pl.ds(0, SEATS), :] = first
            bs[q, pl.ds(SEATS, SEATS), :] = second
            bsm[q] = scores
            home_meta(q, zi).start()
            home_copy(q, zi).start()

    half = ny // 2

    def order(i):
        d = lax.div(i + 1, 2)
        return at_y(jnp.where(lax.rem(i, 2) == 1, -d, d))

    done = 0
    mixed = 0
    for s in range(1, half + 2):
        if s <= half:
            for j, way in flows:
                if s > hops[j, way]:
                    continue
                q = ag_wait(j, way, s)
                if s + 1 <= hops[j, way]:
                    ag_copy(j, way, s + 1).start()
                half_copy(q, j, ci).start()
        upto = 1 if s == 1 else min(2 * s - 1, ny) if s <= half else ny

        def step(i, _):
            consume(order(i))
            return 0

        lax.fori_loop(done, upto, step, 0)
        done = upto
        ready = max(0, upto - 3) if s <= half else ny

        def join(i, _):
            combine(order(i))
            return 0

        lax.fori_loop(mixed, ready, join, 0)
        mixed = ready

    def seat_x(q, _):
        for d in range(1, NX):
            xs = lax.rem(xi + d, NX)
            x_copy(XT, q, xs, xs).wait_recv()
        moved = dot(perm[q], rx[XT, q].reshape(NX * SEATS, -1)).astype(BF16)
        slots[XT, 0, q] = moved[:ROWS]
        slots[XT, 1, q] = moved[ROWS:]
        return 0

    lax.fori_loop(0, nz, seat_x, 0)

    def weight_grads(j, _):
        x = slots[XT, j].reshape(nz * ROWS, -1)
        gg_ref[j] = dot(x, dg[j].reshape(nz * ROWS, -1), 0, 0).astype(BF16)
        ug_ref[j] = dot(x, du[j].reshape(nz * ROWS, -1), 0, 0).astype(BF16)
        return 0

    lax.fori_loop(0, 2, weight_grads, 0)

    def wait_home(k, _):
        q = lax.rem(zi + k, nz)
        home_meta(q, q).wait_recv()
        home_copy(q, q).wait_recv()
        return 0

    lax.fori_loop(1, nz, wait_home, 0)
    tg_ref[...] = dot(gmat[...], br[...].reshape(nz * 2 * SEATS, -1), 0, 0).astype(BF16)
    scores = jnp.concatenate([brm[q] for q in range(nz)], axis=1)
    hi = scores.astype(BF16)
    rest1 = scores - hi.astype(F32)
    mid = rest1.astype(BF16)
    low = (rest1 - mid.astype(F32)).astype(BF16)
    g = gmat[...]
    picked = dot(hi, g) + dot(mid, g) + dot(low, g)
    line = lax.broadcasted_iota(jnp.int32, picked.shape, 0)
    rg_ref[0:1, :] = jnp.sum(jnp.where(line == (id0 & 3), picked, 0.0), axis=0, keepdims=True)
    rg_ref[1:2, :] = jnp.sum(jnp.where(line == (id1 & 3), picked, 0.0), axis=0, keepdims=True)

    def drain_z(k, _):
        zt = lax.rem(zi + k, nz)
        for which in (META, DY, XT):
            z_copy(which, zt, zi).wait_send()
        home_meta(zt, zi).wait_send()
        home_copy(zt, zi).wait_send()
        return 0

    lax.fori_loop(1, nz, drain_z, 0)

    def drain_q(q, _):
        for d in range(1, NX):
            xt = lax.rem(xi + d, NX)
            for which in (META, DY, XT):
                x_copy(which, q, xt, xi).wait_send()
            back_meta(q, xt, xi).wait_send()
            back_copy(q, xt, xi).wait_send()
        pair_copy(q).wait_send()
        for j in range(2):
            half_copy(q, j, ci).wait_send()
        return 0

    lax.fori_loop(0, nz, drain_q, 0)
    for j, way in flows:
        for s in range(1, hops[j, way] + 1):
            rs_copy(j, way, s).wait_send()
            ag_copy(j, way, s).wait_send()


def local(nz, ids, rw, tok, cot, gate, up, down, sg, su):
    tokens, wide = tok.shape
    f = gate.shape[-1]
    hf = f // 2
    ny = nz
    experts = 8 * nz
    vm = pltpu.VMEM
    dma = pltpu.SemaphoreType.DMA
    steps = max(ny // 2, 1)
    scratch = [
        vm(gate.shape, BF16), vm(up.shape, BF16), vm(down.shape, BF16),
        vm(sg.shape, BF16), vm(su.shape, BF16),
        vm((2, nz, ROWS, f), F32), vm((2, nz, ROWS, f), F32), vm((2, nz, ROWS, f), F32),
        vm((3, experts, tokens), F32), vm((nz * 2 * SEATS, tokens), BF16),
        vm((2, nz, 2 * SEATS, wide), BF16), vm((nz, 8, 128), F32),
        vm((2, nz, 2 * SEATS, wide), BF16), vm((nz, 8, 128), F32),
        vm((2, nz, NX, SEATS, wide), BF16), vm((nz, NX, 8, 128), F32),
        vm((nz, 2 * ROWS, NX * SEATS), BF16), vm((2, nz, ROWS, 128), F32),
        vm((2, 2, nz, ROWS, wide), BF16),
        vm((nz, 2, 2, ROWS, hf), BF16), vm((nz, 2, ROWS, hf), BF16),
        vm((2, 2, steps, ROWS, hf), BF16), vm((2, 2, steps, ROWS, hf), BF16),
        vm((nz, 2, 2, ROWS, hf), BF16),
        vm((2, nz, ROWS, f), BF16), vm((2, nz, ROWS, f), BF16),
        vm((nz, NX, SEATS, wide), BF16), vm((nz, NX, 8, 128), F32),
        vm((nz, NX, SEATS, wide), BF16), vm((nz, NX, 8, 128), F32),
        vm((nz, 2 * SEATS, wide), BF16), vm((nz, 8, 128), F32),
        vm((nz, 2 * SEATS, wide), BF16), vm((nz, 8, 128), F32),
        dma((5,)), dma((3, nz)), dma((3, nz)), dma((3, nz, NX)), dma((3, nz, NX)),
        dma((nz,)), dma((nz,)), dma((2, 2, steps)), dma((2, 2, steps)),
        dma((2, 2, steps)), dma((2, 2, steps)), dma((nz, 2)), dma((nz, 2)),
        dma((2, nz, NX)), dma((2, nz, NX)), dma((2, nz)), dma((2, nz)),
    ]
    inside = pl.BlockSpec(memory_space=pltpu.VMEM)
    outside = pl.BlockSpec(memory_space=pl.ANY)
    out = pl.pallas_call(
        functools.partial(kernel, nz),
        out_shape=(
            jax.ShapeDtypeStruct(tok.shape, BF16),
            jax.ShapeDtypeStruct((2, tokens), F32),
            jax.ShapeDtypeStruct(gate.shape, BF16),
            jax.ShapeDtypeStruct(up.shape, BF16),
            jax.ShapeDtypeStruct(down.shape, BF16),
        ),
        in_specs=[inside] * 4 + [outside] * 5,
        out_specs=(inside,) * 5,
        scratch_shapes=scratch,
        compiler_params=pltpu.CompilerParams(
            collective_id=0, has_side_effects=True, vmem_limit_bytes=60 * 1024 * 1024
        ),
    )(ids.T, rw.T, tok, cot, gate, up, down, sg, su)
    return (out[0], out[1].T, *out[2:])


def on_axes(mesh, nz):
    return jax.shard_map(
        functools.partial(
            lambda n, tok, cot, ids, rw, *others: local(n, ids, rw, tok, cot, *others), nz
        ),
        mesh=mesh,
        in_specs=(
            P(EP, TP), P(EP, TP), P(EP, None), P(EP, None),
            P(EP, TP, None), P(EP, TP, None), P(EP, None, TP),
            P(None, EP, None, None), P(None, EP, None, None),
        ),
        out_specs=(
            P(EP, TP), P(EP, None), P(EP, TP, None), P(EP, TP, None), P(EP, None, TP),
        ),
        check_vma=False,
    )


def solution(mesh):
    nz = mesh.shape["ep"] // NX
    return on_axes(Mesh(mesh.devices.reshape(nz, NX, nz, 2), ("z", "x", "y", "c")), nz)
```

```python
import functools

import jax
import jax.numpy as jnp
from jax import lax
from jax.experimental import pallas as pl
from jax.experimental.pallas import tpu as pltpu
from jax.sharding import Mesh
from jax.sharding import PartitionSpec as P

EP = ("z", "x")
TP = ("y", "c")
NX = 4
CAP = 32
SEATS = 64
ROWS = NX * CAP
F32 = jnp.float32
BF16 = jnp.bfloat16
DY, XT, META = 0, 1, 2


def dot(a, b, ca=1, cb=0):
    return lax.dot_general(a, b, (((ca,), (cb,)), ((), ())), preferred_element_type=F32)


def kernel(
    nz, ids_hbm, rw_hbm, tok_hbm, cot_hbm, gate_hbm, up_hbm, down_hbm, sg_hbm, su_hbm,
    tg_hbm, rg_hbm, gg_hbm, ug_hbm, dg_hbm,
    ids_ref, rw_ref, tok_ref, cot_ref, gate, up, down, sg, su,
    tg_ref, rg_ref, gg_ref, ug_ref, dg_ref, pre_u, pre_g, hid, hw, pw, gmat,
    sz, szm, rz, rzm, rx, rxm, perm, wcol, slots,
    zp, zr, rss, rsr, zf, du, dg, ts, tsm, cx, cxm, bs, bsm, br, brm,
    lsem, osem, zss, zrs, xss, xrs, xtr, pss, prs, rcs, rcr, acs, acr, qss, qrs, vss, vrs, wss, wrs,
):
    zi, xi, yi, ci = (lax.axis_index(a) for a in ("z", "x", "y", "c"))
    ny = nz
    part_n = nz // 2
    hf = zf.shape[-1]
    tokens = tok_ref.shape[0]
    left_half = lax.div(xi, 2) == 0
    my_row = 2 * lax.rem(xi, 2)
    seat0 = pl.multiple_of(SEATS * lax.div(xi, 2), SEATS)

    def near_first(k):
        k = jnp.int32(k)
        return jnp.where(lax.rem(k, 2) == 1, lax.div(k + 1, 2), nz - lax.div(k, 2))

    def came(k):
        return lax.rem(zi + 2 * nz - near_first(k), nz)

    def remote(src, dst, ssem, rsem, **where):
        return pltpu.make_async_remote_copy(
            src_ref=src, dst_ref=dst, send_sem=ssem, recv_sem=rsem,
            device_id=where, device_id_type=pl.DeviceIdType.MESH,
        )

    barrier = pltpu.get_barrier_semaphore()

    def greet(**where):
        pl.semaphore_signal(barrier, 1, device_id=where, device_id_type=pl.DeviceIdType.MESH)

    for k in range(1, nz):
        greet(z=lax.rem(zi + k, nz))
    for k in range(1, NX):
        greet(x=lax.rem(xi + k, NX))
    greet(y=lax.rem(yi + 1, ny))
    greet(y=lax.rem(yi + ny - 1, ny))
    greet(c=1 - ci)

    loads = [
        pltpu.make_async_copy(src, dst, lsem.at[i])
        for i, (src, dst) in enumerate(
            (
                (ids_hbm, ids_ref), (rw_hbm, rw_ref), (cot_hbm, cot_ref), (tok_hbm, tok_ref),
                (down_hbm, down), (sg_hbm, sg), (su_hbm, su), (gate_hbm, gate), (up_hbm, up),
            )
        )
    ]
    results = [
        pltpu.make_async_copy(src, dst, osem.at[i])
        for i, (src, dst) in enumerate(
            (
                (tg_ref, tg_hbm), (rg_ref, rg_hbm), (gg_ref, gg_hbm),
                (ug_ref, ug_hbm), (dg_ref, dg_hbm),
            )
        )
    ]
    for copy in loads:
        copy.start()
    loads[0].wait()
    loads[1].wait()

    experts, groups = 4 * 2 * nz, 2 * nz
    id0, id1 = ids_ref[0:1, :], ids_ref[1:2, :]
    rw0, rw1 = rw_ref[0:1, :], rw_ref[1:2, :]
    group = lax.shift_right_logical(id0, 2)
    erow = lax.broadcasted_iota(jnp.int32, (experts, tokens), 0)
    hot0, hot1 = erow == id0, erow == id1
    chosen = jnp.where(hot0, 1.0, 0.0) + jnp.where(hot1, 1.0, 0.0)
    grow = lax.broadcasted_iota(jnp.int32, (groups, tokens), 0)
    ingroup = jnp.where(grow == group, 1.0, 0.0)
    earlier = jnp.where(
        lax.broadcasted_iota(jnp.int32, (tokens, tokens), 0)
        < lax.broadcasted_iota(jnp.int32, (tokens, tokens), 1),
        1.0, 0.0,
    ).astype(BF16)
    count = dot(jnp.concatenate([chosen, ingroup], axis=0).astype(BF16), earlier)
    rank = jnp.sum(ingroup * count[experts:], axis=0, keepdims=True)
    target = group * SEATS + rank.astype(jnp.int32)
    weight = jnp.where(hot0, rw0, 0.0) + jnp.where(hot1, rw1, 0.0)
    weight_hi = weight.astype(BF16).astype(F32)
    pw[0] = chosen * (count[:experts] + 1.0)
    pw[1] = weight_hi
    pw[2] = weight - weight_hi

    def seat_rows(zt):
        row = lax.broadcasted_iota(jnp.int32, (2 * SEATS, tokens), 0) + zt * (2 * SEATS)
        return jnp.where(row == target, 1.0, 0.0).astype(BF16)

    def gathered(zt):
        g = seat_rows(zt)
        gmat[pl.ds(pl.multiple_of(zt * 2 * SEATS, 2 * SEATS), 2 * SEATS), :] = g
        e0 = pl.multiple_of(zt * 8, 8)
        lhs = jnp.concatenate([pw[i, pl.ds(e0, 8), :] for i in range(3)], axis=0).astype(BF16)
        r = dot(lhs, g, 1, 1)
        tile = jnp.concatenate(
            [r[0:4] + r[4:8], (r[8:12] + r[12:16]) + (r[16:20] + r[20:24])], axis=0
        )
        return dot(g, cot_ref[...]).astype(BF16), tile

    loads[2].wait()
    rows, tile = gathered(zi)
    rz[DY, zi] = rows
    rzm[zi] = tile

    def z_copy(which, zt, zs):
        if which == META:
            return remote(szm.at[zt], rzm.at[zs], zss.at[META], zrs.at[META, zs], z=zt)
        return remote(sz.at[which, zt], rz.at[which, zs], zss.at[which], zrs.at[which, zs], z=zt)

    def x_copy(which, q, xt, xs):
        if which == META:
            return remote(rzm.at[q], rxm.at[q, xs], xss.at[META], xrs.at[1, q], x=xt)
        seats = pl.ds(pl.multiple_of(SEATS * lax.div(xt, 2), SEATS), SEATS)
        return remote(
            rz.at[which, q, seats], rx.at[which, q, xs],
            xss.at[which], xtr.at[0] if which == XT else xrs.at[0, q], x=xt,
        )

    def spread(which, q):
        for d in range(1, NX):
            x_copy(which, q, lax.rem(xi + d, NX), xi).start()

    def pass_dy(q):
        spread(META, q)
        spread(DY, q)
        rx[DY, q, xi] = rz[DY, q, pl.ds(seat0, SEATS), :]
        rxm[q, xi] = rzm[q]

    def send_dy(k, _):
        zt = lax.rem(zi + near_first(k), nz)
        rows, tile = gathered(zt)
        szm[zt] = tile
        sz[DY, zt] = rows
        z_copy(META, zt, zi).start()
        z_copy(DY, zt, zi).start()
        return 0

    pl.semaphore_wait(barrier, (nz - 1) + (NX - 1) + 3)

    lax.fori_loop(1, nz, send_dy, 0)
    pass_dy(zi)

    def rows_of_tokens(zt):
        g = gmat[pl.ds(pl.multiple_of(zt * 2 * SEATS, 2 * SEATS), 2 * SEATS), :]
        return dot(g, tok_ref[...]).astype(BF16)

    def send_x(k, _):
        zt = lax.rem(zi + near_first(k), nz)
        sz[XT, zt] = rows_of_tokens(zt)
        z_copy(XT, zt, zi).start()
        return 0

    def elementwise(i, _):
        q, j = lax.div(i, 2), lax.rem(i, 2)
        g = sg[pl.ds(NX * q, NX), j].astype(F32).reshape(ROWS, -1)
        u = su[pl.ds(NX * q, NX), j].astype(F32).reshape(ROWS, -1)
        s = jax.nn.sigmoid(g)
        gs = g * s
        pre_u[j, q] = gs
        pre_g[j, q] = u * s * (1.0 + g * (1.0 - s))
        hid[j, q] = gs * u
        return 0

    def take_dy(k):
        q = came(k)
        z_copy(META, q, q).wait_recv()
        z_copy(DY, q, q).wait_recv()
        pass_dy(q)

    def pair_copy(q, h):
        return remote(zp.at[q, 1 - ci], zr.at[q], pss.at[0], prs.at[h], c=1 - ci)

    def back_partial(k):
        q = came(k)
        metas, rows = rxm.at[q, pl.ds(0, NX - 1)], rx.at[DY, q, pl.ds(0, NX - 1)]
        remote(metas, metas, xss.at[META], xrs.at[1, q], c=1 - ci).wait_recv()
        remote(rows, rows, xss.at[DY], xrs.at[0, q], c=1 - ci).wait_recv()
        t = rxm[q]
        t = jnp.where(left_half, t[:, :, :SEATS], t[:, :, SEATS:])
        line = lax.broadcasted_iota(jnp.int32, t.shape, 1)

        def lanes(i):
            v = jnp.sum(jnp.where(line == i, t, 0.0), axis=1)
            return jnp.concatenate([v[n : n + 1] for n in range(NX)], axis=1)

        base = CAP * lax.div(lax.broadcasted_iota(jnp.int32, (1, NX * SEATS), 1), SEATS)
        slot = lax.broadcasted_iota(jnp.int32, (ROWS, NX * SEATS), 0)
        for j in range(2):
            place = lanes(my_row + j).astype(jnp.int32)
            key = jnp.where(place > 0, place - 1 + base, -1)
            hit = slot == key
            perm[q, pl.ds(j * ROWS, ROWS), :] = jnp.where(hit, 1.0, 0.0).astype(BF16)
            w = jnp.sum(jnp.where(hit, lanes(4 + my_row + j), 0.0), axis=1, keepdims=True)
            wcol[j, q] = jnp.broadcast_to(w, (ROWS, 128))
        arrived = rx[DY, q].reshape(NX * SEATS, -1)
        moved = dot(perm[q], arrived).astype(BF16)
        for j in range(2):
            part = moved[j * ROWS : (j + 1) * ROWS]
            slots[DY, j, q] = part
            z = dot(part, down[j], 1, 1).astype(BF16)
            zp[q, 0, j] = z[:, :hf]
            zp[q, 1, j] = z[:, hf:]
        pair_copy(q, k // part_n).start()

    piece = ROWS // 2
    half_y = ny // 2
    hops = {
        (0, 0): half_y, (0, 1): ny - 1 - half_y, (1, 0): ny - 1 - half_y, (1, 1): half_y,
    }
    flows = list(hops)

    def at_y(d):
        return lax.rem(yi + d + 2 * ny, ny)

    def unit(h, d):
        return came(part_n * h + lax.div(d, 2)), lax.rem(d, 2)

    def own(h, d, p):
        q, j = unit(h, d)
        rows = pl.ds(p * piece, piece)
        return zp[q, ci, j, rows, :].astype(F32) + zr[q, j, rows, :].astype(F32)

    def rs_copy(h, p, way, s):
        return remote(
            rss.at[h, p, way, s - 1], rsr.at[h, p, way, s - 1],
            rcs.at[h, p, way], rcr.at[h, p, way, s - 1], y=at_y(1 - 2 * way),
        )

    def rs_step(h, s):
        for p, way in flows:
            if s > hops[p, way]:
                continue
            total = own(h, at_y((1 - 2 * way) * (hops[p, way] + 1 - s)), p)
            if s > 1:
                rs_copy(h, p, way, s - 1).wait_recv()
                total = total + rsr[h, p, way, s - 2].astype(F32)
            rss[h, p, way, s - 1] = total.astype(BF16)
            rs_copy(h, p, way, s).start()

    def ag_copy(h, p, way, s):
        step = 1 - 2 * way
        q, j = unit(h, at_y(-step * (s - 1)))
        spot = zf.at[q, ci, j, pl.ds(p * piece, piece)]
        return remote(
            spot, spot, acs.at[h, p, way], acr.at[h, p, way, s - 1], y=at_y(step)
        )

    def ag_wait(h, p, way, s):
        q, j = unit(h, at_y(-(1 - 2 * way) * s))
        spot = zf.at[q, ci, j, pl.ds(p * piece, piece)]
        remote(
            spot, spot, acs.at[h, p, way], acr.at[h, p, way, s - 1], y=at_y(1)
        ).wait_recv()

    def half_copy(q, j, c):
        spot = zf.at[q, c, j]
        return remote(spot, spot, qss.at[0], qrs.at[q], c=1 - ci)

    def rs_end(h):
        q, j = unit(h, yi)
        for p in range(2):
            total = own(h, yi, p)
            for way in range(2):
                if hops[p, way] > 0:
                    rs_copy(h, p, way, hops[p, way]).wait_recv()
                    total = total + rsr[h, p, way, hops[p, way] - 1].astype(F32)
            zf[q, ci, j, pl.ds(p * piece, piece), :] = total.astype(BF16)
        for p, way in flows:
            if hops[p, way] > 0:
                ag_copy(h, p, way, 1).start()
        half_copy(q, j, ci).start()

    def ag_step(h, s):
        for p, way in flows:
            if s > hops[p, way]:
                continue
            ag_wait(h, p, way, s)
            if s + 1 <= hops[p, way]:
                ag_copy(h, p, way, s + 1).start()
        for d in (-s, s) if 2 * s < ny else (s,):
            q, j = unit(h, at_y(d))
            half_copy(q, j, ci).start()

    def take_x(k):
        q = came(k)
        if not (isinstance(k, int) and k == 0):
            z_copy(XT, q, q).wait_recv()
        spread(XT, q)
        rx[XT, q, xi] = rz[XT, q, pl.ds(seat0, SEATS), :]

    def back_copy(q, xt, xs):
        return remote(ts.at[q, xt], cx.at[q, xs], vss.at[0], vrs.at[0, q], x=xt)

    def back_meta(q, xt, xs):
        return remote(tsm.at[q, xt], cxm.at[q, xs], vss.at[1], vrs.at[1, q], x=xt)

    def consume(q):
        both = zf.at[q, 1 - ci]
        remote(both, both, qss.at[0], qrs.at[q], c=1 - ci).wait_recv()
        grads, tiles = [], None
        line = lax.broadcasted_iota(jnp.int32, (8, 2 * SEATS), 0)
        side = lax.div(lax.broadcasted_iota(jnp.int32, (8, 2 * SEATS), 1), SEATS) == lax.div(xi, 2)
        for j in range(2):
            z = jnp.concatenate([zf[q, 0, j], zf[q, 1, j]], axis=1).astype(F32)
            w = jnp.concatenate([wcol[j, q]] * (z.shape[-1] // 128), axis=1)
            wz = w * z
            up_grad = (wz * pre_u[j, q]).astype(BF16)
            gate_grad = (wz * pre_g[j, q]).astype(BF16)
            du[j, q] = up_grad
            dg[j, q] = gate_grad
            hb = hid[j, q].astype(BF16).astype(F32)
            score = jnp.sum(hb * z, axis=1, keepdims=True)
            p = perm[q, pl.ds(j * ROWS, ROWS), :].astype(F32)
            seat_score = jnp.sum(p * score, axis=0, keepdims=True)
            s = dot(gate_grad, gate[j], 1, 1) + dot(up_grad, up[j], 1, 1)
            grads.append(s.astype(BF16))
            mask = side & (line == my_row + j)
            made = []
            for n in range(NX):
                one = seat_score[:, n * SEATS : (n + 1) * SEATS]
                made.append(jnp.where(mask, jnp.concatenate([one, one], axis=1), 0.0))
            tiles = made if tiles is None else [a + b for a, b in zip(tiles, made)]
        for n in range(NX):
            tsm[q, n] = tiles[n]
        t = dot(perm[q], jnp.concatenate(grads, axis=0), 0, 0).astype(BF16)
        ts[q] = t.reshape(NX, SEATS, -1)
        for d in range(1, NX):
            xt = lax.rem(xi + d, NX)
            back_meta(q, xt, xi).start()
            back_copy(q, xt, xi).start()
        cx[q, xi] = ts[q, xi]
        cxm[q, xi] = tsm[q, xi]

    def home_copy(q, zs):
        return remote(bs.at[q], br.at[zs], wss.at[0], wrs.at[0], z=q)

    def home_meta(q, zs):
        return remote(bsm.at[q], brm.at[zs], wss.at[1], wrs.at[1], z=q)

    def combine(q):
        metas, rows = cxm.at[q, pl.ds(0, NX - 1)], cx.at[q, pl.ds(0, NX - 1)]
        remote(metas, metas, vss.at[1], vrs.at[1, q], c=1 - ci).wait_recv()
        remote(rows, rows, vss.at[0], vrs.at[0, q], c=1 - ci).wait_recv()
        first = (cx[q, 0].astype(F32) + cx[q, 1].astype(F32)).astype(BF16)
        second = (cx[q, 2].astype(F32) + cx[q, 3].astype(F32)).astype(BF16)
        scores = (cxm[q, 0] + cxm[q, 1]) + (cxm[q, 2] + cxm[q, 3])

        @pl.when(q == zi)
        def _():
            br[q, pl.ds(0, SEATS), :] = first
            br[q, pl.ds(SEATS, SEATS), :] = second
            brm[q] = scores

        @pl.when(q != zi)
        def _():
            bs[q, pl.ds(0, SEATS), :] = first
            bs[q, pl.ds(SEATS, SEATS), :] = second
            bsm[q] = scores
            home_meta(q, zi).start()
            home_copy(q, zi).start()

    def turn(h, i):
        d = (i + 1) // 2
        even = lax.rem(yi, 2) == 0
        shift = jnp.where(even, d, -d) if i % 2 == 0 else jnp.where(even, -d, d)
        return came(part_n * h + lax.rem(lax.div(yi, 2) + shift + 2 * part_n, part_n))

    def down_grads(j):
        def weigh(q, _):
            w = jnp.concatenate([wcol[j, q]] * (hid.shape[-1] // 128), axis=1)
            hw[j, q] = (w * hid[j, q]).astype(BF16)
            return 0

        lax.fori_loop(0, nz, weigh, 0)
        weighted = hw[j].reshape(nz * ROWS, -1)
        dy = slots[DY, j].reshape(nz * ROWS, -1)
        dg_ref[j] = dot(weighted, dy, 0, 0).astype(BF16)

    def wait_pairs(h):
        span = zr.at[pl.ds(0, part_n)]
        remote(span, span, pss.at[0], prs.at[h], c=1 - ci).wait_recv()

    loads[5].wait()
    loads[6].wait()
    lax.fori_loop(0, 2 * nz, elementwise, 0)

    loads[4].wait()
    for k in range(1, part_n):
        take_dy(k)
        back_partial(k - 1)
    back_partial(part_n - 1)

    wait_pairs(0)
    rs_step(0, 1)
    for k in range(part_n, nz):
        take_dy(k)
    loads[3].wait()
    lax.fori_loop(1, nz, send_x, 0)
    rz[XT, zi] = rows_of_tokens(zi)
    backs = list(range(part_n, nz))
    for s in range(2, half_y):
        rs_step(0, s)
        for _ in range(2):
            if backs:
                back_partial(backs.pop(0))
    while backs:
        back_partial(backs.pop(0))
    if half_y > 1:
        rs_step(0, half_y)
    wait_pairs(1)
    rs_step(1, 1)
    rs_end(0)
    loads[7].wait()
    loads[8].wait()
    for s in range(2, half_y + 1):
        rs_step(1, s)
        ag_step(0, s - 1)
        if s == 2:
            for k in range(part_n):
                take_x(k)
            down_grads(0)
        else:
            consume(turn(0, s - 3))
            down_grads(1) if s == 3 else None
    rs_end(1)
    for k in range(part_n if half_y > 1 else 0, nz):
        take_x(k)
    if half_y < 2:
        down_grads(0)
    if half_y < 3:
        down_grads(1)
    results[4].start()
    ag_step(0, half_y)
    for i in range(max(half_y - 2, 0), part_n):
        consume(turn(0, i))
    for s in range(1, half_y + 1):
        ag_step(1, s)
        if s > 1:
            consume(turn(1, s - 2))
        combine(turn(0, s - 1))
    consume(turn(1, part_n - 1))
    for i in range(part_n):
        combine(turn(1, i))

    def seat_x(q, _):
        moved = dot(perm[q], rx[XT, q].reshape(NX * SEATS, -1)).astype(BF16)
        slots[XT, 0, q] = moved[:ROWS]
        slots[XT, 1, q] = moved[ROWS:]
        return 0

    x_rows = rx.at[XT, pl.ds(0, nz), pl.ds(0, NX - 1)]
    remote(x_rows, x_rows, xss.at[XT], xtr.at[0], c=1 - ci).wait_recv()
    lax.fori_loop(0, nz, seat_x, 0)

    def weight_grads(j, _):
        x = slots[XT, j].reshape(nz * ROWS, -1)
        gg_ref[j] = dot(x, dg[j].reshape(nz * ROWS, -1), 0, 0).astype(BF16)
        ug_ref[j] = dot(x, du[j].reshape(nz * ROWS, -1), 0, 0).astype(BF16)
        return 0

    lax.fori_loop(0, 2, weight_grads, 0)
    results[2].start()
    results[3].start()

    def gone(span, sem):
        remote(span, span, sem, sem, c=1 - ci).wait_send()

    def came_in(span, sem):
        remote(span, span, sem, sem, c=1 - ci).wait_recv()

    gone(szm.at[pl.ds(0, nz - 1)], zss.at[META])
    gone(rxm.at[pl.ds(0, nz), pl.ds(0, NX - 1)], xss.at[META])
    for which in (DY, XT):
        gone(sz.at[which, pl.ds(0, nz - 1)], zss.at[which])
        gone(rx.at[which, pl.ds(0, nz), pl.ds(0, NX - 1)], xss.at[which])
    gone(ts.at[pl.ds(0, nz), pl.ds(0, NX - 1)], vss.at[0])
    gone(tsm.at[pl.ds(0, nz), pl.ds(0, NX - 1)], vss.at[1])
    gone(zr, pss.at[0])
    gone(zr, qss.at[0])
    for h in range(2):
        for p, way in flows:
            if hops[p, way] > 0:
                gone(rss.at[h, p, way, pl.ds(0, hops[p, way])], rcs.at[h, p, way])
                gone(rss.at[h, p, way, pl.ds(0, hops[p, way])], acs.at[h, p, way])

    came_in(brm.at[pl.ds(0, nz - 1)], wrs.at[1])
    came_in(br.at[pl.ds(0, nz - 1)], wrs.at[0])
    tg_ref[...] = dot(gmat[...], br[...].reshape(nz * 2 * SEATS, -1), 0, 0).astype(BF16)
    results[0].start()
    scores = jnp.concatenate([brm[q] for q in range(nz)], axis=1)
    hi = scores.astype(BF16)
    rest1 = scores - hi.astype(F32)
    mid = rest1.astype(BF16)
    low = (rest1 - mid.astype(F32)).astype(BF16)
    g = gmat[...]
    picked = dot(hi, g) + dot(mid, g) + dot(low, g)
    line = lax.broadcasted_iota(jnp.int32, picked.shape, 0)
    rg_ref[0:1, :] = jnp.sum(jnp.where(line == (id0 & 3), picked, 0.0), axis=0, keepdims=True)
    rg_ref[1:2, :] = jnp.sum(jnp.where(line == (id1 & 3), picked, 0.0), axis=0, keepdims=True)
    results[1].start()

    gone(bsm.at[pl.ds(0, nz - 1)], wss.at[1])
    gone(bs.at[pl.ds(0, nz - 1)], wss.at[0])
    for copy in results:
        copy.wait()


def forward(*refs):
    n = 5
    froms, tos, held = refs[:n], refs[n : 2 * n], refs[2 * n : 3 * n]
    came, gone = refs[3 * n :]
    ins = [pltpu.make_async_copy(froms[i], held[i], came.at[i]) for i in range(n)]
    outs = [pltpu.make_async_copy(held[i], tos[i], gone.at[i]) for i in range(n)]
    for copy in ins:
        copy.start()
    for i in range(n):
        ins[i].wait()
        outs[i].start()
    for copy in outs:
        copy.wait()


def local(nz, ids, rw, tok, cot, gate, up, down, sg, su):
    tokens, wide = tok.shape
    f = gate.shape[-1]
    hf = f // 2
    ny = nz
    experts = 8 * nz
    vm = pltpu.VMEM
    dma = pltpu.SemaphoreType.DMA
    steps = max(ny // 2, 1)
    piece = ROWS // 2
    shapes = (
        jax.ShapeDtypeStruct(tok.shape, BF16),
        jax.ShapeDtypeStruct((2, tokens), F32),
        jax.ShapeDtypeStruct(gate.shape, BF16),
        jax.ShapeDtypeStruct(up.shape, BF16),
        jax.ShapeDtypeStruct(down.shape, BF16),
    )
    held = [vm(s.shape, s.dtype) for s in shapes]
    scratch = [
        vm((2, tokens), jnp.int32), vm((2, tokens), F32), vm(tok.shape, BF16), vm(cot.shape, BF16),
        vm(gate.shape, BF16), vm(up.shape, BF16), vm(down.shape, BF16),
        vm(sg.shape, BF16), vm(su.shape, BF16), *held,
        vm((2, nz, ROWS, f), F32), vm((2, nz, ROWS, f), F32), vm((2, nz, ROWS, f), F32),
        vm((2, nz, ROWS, f), BF16),
        vm((3, experts, tokens), F32), vm((nz * 2 * SEATS, tokens), BF16),
        vm((2, nz, 2 * SEATS, wide), BF16), vm((nz, 8, 128), F32),
        vm((2, nz, 2 * SEATS, wide), BF16), vm((nz, 8, 128), F32),
        vm((2, nz, NX, SEATS, wide), BF16), vm((nz, NX, 8, 128), F32),
        vm((nz, 2 * ROWS, NX * SEATS), BF16), vm((2, nz, ROWS, 128), F32),
        vm((2, 2, nz, ROWS, wide), BF16),
        vm((nz, 2, 2, ROWS, hf), BF16), vm((nz, 2, ROWS, hf), BF16),
        vm((2, 2, 2, steps, piece, hf), BF16), vm((2, 2, 2, steps, piece, hf), BF16),
        vm((nz, 2, 2, ROWS, hf), BF16),
        vm((2, nz, ROWS, f), BF16), vm((2, nz, ROWS, f), BF16),
        vm((nz, NX, SEATS, wide), BF16), vm((nz, NX, 8, 128), F32),
        vm((nz, NX, SEATS, wide), BF16), vm((nz, NX, 8, 128), F32),
        vm((nz, 2 * SEATS, wide), BF16), vm((nz, 8, 128), F32),
        vm((nz, 2 * SEATS, wide), BF16), vm((nz, 8, 128), F32),
        dma((9,)), dma((5,)), dma((3,)), dma((3, nz)), dma((3,)), dma((2, nz)), dma((1,)),
        dma((1,)), dma((2,)), dma((2, 2, 2)), dma((2, 2, 2, steps)),
        dma((2, 2, 2)), dma((2, 2, 2, steps)), dma((1,)), dma((nz,)),
        dma((2,)), dma((2, nz)), dma((2,)), dma((2,)),
    ]
    outside = pl.BlockSpec(memory_space=pl.ANY)
    made = pl.pallas_call(
        functools.partial(kernel, nz),
        out_shape=shapes,
        in_specs=[outside] * 9,
        out_specs=(outside,) * 5,
        scratch_shapes=scratch,
        compiler_params=pltpu.CompilerParams(
            collective_id=0, has_side_effects=True, vmem_limit_bytes=60 * 1024 * 1024
        ),
    )(ids.T, rw.T, tok, cot, gate, up, down, sg, su)
    out = pl.pallas_call(
        forward,
        out_shape=shapes,
        in_specs=[outside] * 5,
        out_specs=(outside,) * 5,
        scratch_shapes=[*held, dma((5,)), dma((5,))],
        compiler_params=pltpu.CompilerParams(vmem_limit_bytes=60 * 1024 * 1024),
    )(*made)
    return (out[0], out[1].T, *out[2:])


def on_axes(mesh, nz):
    return jax.shard_map(
        functools.partial(
            lambda n, tok, cot, ids, rw, *others: local(n, ids, rw, tok, cot, *others), nz
        ),
        mesh=mesh,
        in_specs=(
            P(EP, TP), P(EP, TP), P(EP, None), P(EP, None),
            P(EP, TP, None), P(EP, TP, None), P(EP, None, TP),
            P(None, EP, None, None), P(None, EP, None, None),
        ),
        out_specs=(
            P(EP, TP), P(EP, None), P(EP, TP, None), P(EP, TP, None), P(EP, None, TP),
        ),
        check_vma=False,
    )


def solution(mesh):
    nz = mesh.shape["ep"] // NX
    return on_axes(Mesh(mesh.devices.reshape(nz, NX, nz, 2), ("z", "x", "y", "c")), nz)
```
